32 devices in a mesh: grp: 2 (over y), sp: 4 (over z), tp: 4 (over x, core).
Axes of the slice: x: 2, y: 2, z: 4, core: 2. Of those that a mesh axis runs over, the one named last changes fastest.
Arguments:
- tokens: bfloat16 [8, 512, 4096], P('grp', 'sp'), parts along dimension 0, may hold values from -9 to 9
- w_forget: bfloat16 [4096, 4096], P('sp', 'tp'), may hold values from -0.09375 to 0.09375
- w_value: bfloat16 [4096, 4096], P('sp', 'tp'), may hold values from -0.09375 to 0.09375
- lower_bound: float32 [4096], P('tp'), may hold values from 0.25 to 1
- decay_shift: float32 [8, 512, 32], P('grp', 'sp', 'tp'), parts along dimension 0, may hold values from -1 to 0
- queries: bfloat16 [8, 4096], P('grp', 'tp'), parts along dimension 0, may hold values from -6 to 6
- read_gain: float32 [4096], P('tp'), may hold values from 0.1 to 1.9
Outputs:
- cache_out: bfloat16 [8, 32, 16384], P('grp', 'tp', 'sp'), parts along dimension 0
- first_read: bfloat16 [8, 4096], P('grp', 'tp'), parts along dimension 0
The draws below stay inside these ranges and needn't reach their ends.
There are 2 independent parts, one for each index of `grp`. The reference program is written for one: setup_inputs(seed, part) draws one part's arguments, and reference() takes and returns one part's arrays. A program takes and returns all parts, laid end to end along the dimension named above; an argument that names none is the same for every part. Nothing has to cross between parts.
All inputs are finite; a program needn't handle non-finite values.
Results may differ from the reference program's by a relative error of at most 0.01.
Values may be sent and summed in bfloat16 or wider, within the bound.
A program may use at most 128 MiB of HBM per device.

```python
import jax
import jax.numpy as jnp
from jax import lax

D = 4096
ATTENTION_UNITS = 32
DK = 128
DV = 128
INPUT_SEQUENCES = 4
SPAN = 128
SEQUENCE_SPAN = 512


def draw_tokens(key, part):
    first_key = jax.random.fold_in(key, 11)
    lookup_vector_two = jax.random.fold_in(key, 12)
    noise_rows = jax.random.normal(first_key, (INPUT_SEQUENCES, SEQUENCE_SPAN, D), jnp.float32)
    block_means = jax.random.normal(lookup_vector_two, (INPUT_SEQUENCES, SEQUENCE_SPAN // SPAN, D), jnp.float32)
    noise_rows = jnp.clip(noise_rows, -5.0, 5.0)
    block_means = jnp.clip(block_means, -4.0, 4.0)
    return (noise_rows + jnp.repeat(block_means, SPAN, axis=1)).astype(jnp.bfloat16)


def draw_lower_bound(key, part):
    first_key = jax.random.fold_in(key, 21)
    lookup_vector_two = jax.random.fold_in(key, 22)
    lookup_vector_three = jax.random.fold_in(key, 23)
    slow_share = 0.5
    slow_heads = jax.random.uniform(first_key, (ATTENTION_UNITS,), jnp.float32) < slow_share
    slow_value = 1.0 - jax.random.uniform(lookup_vector_two, (ATTENTION_UNITS,), jnp.float32, 0.2, 0.6) / SEQUENCE_SPAN
    fast_value = 1.0 - jax.random.uniform(lookup_vector_three, (ATTENTION_UNITS,), jnp.float32, 3.0, 6.0) / SPAN
    bound_heads = jnp.where(slow_heads, slow_value, fast_value)
    return jnp.repeat(bound_heads, DK).astype(jnp.float32)


def draw_decay_shift(key, part):
    first_key = jax.random.fold_in(key, 31)
    lookup_vector_two = jax.random.fold_in(key, 32)
    lookup_vector_three = jax.random.fold_in(key, 33)
    rate_block = jnp.exp(jax.random.uniform(first_key, (INPUT_SEQUENCES, SEQUENCE_SPAN // SPAN, ATTENTION_UNITS), jnp.float32, jnp.log(0.25), jnp.log(1.25)))
    constant_payload = -jnp.repeat(rate_block, SPAN, axis=1) / SEQUENCE_SPAN
    segment_number = jax.random.uniform(lookup_vector_two, (INPUT_SEQUENCES, SEQUENCE_SPAN, ATTENTION_UNITS), jnp.float32) < 2.0 / SEQUENCE_SPAN
    segment_size = jnp.log(jax.random.uniform(lookup_vector_three, (INPUT_SEQUENCES, SEQUENCE_SPAN, ATTENTION_UNITS), jnp.float32, 0.5, 0.8))
    return (constant_payload + jnp.where(segment_number, segment_size, 0.0)).astype(jnp.float32)


def levels(stream_key, dims, cuts, least, top_value):
    def one(dim, shards_of):
        draws = jax.random.uniform(jax.random.fold_in(jax.random.fold_in(stream_key, 6), dim), (shards_of,), jnp.float32, least / len(cuts), top_value / len(cuts))
        return jnp.repeat(jnp.exp(draws), dims[dim] // shards_of).reshape((-1,) + (1,) * (len(dims) - dim - 1))

    gain = one(*cuts[0])
    for cut in cuts[1:]:
        gain = gain * one(*cut)
    return gain


def bell_draw(rng, extent, deviation, reach, cuts=(), dtype=jnp.bfloat16):
    result = jax.random.normal(rng, extent, jnp.float32) * deviation
    if len(cuts) > 0:
        result = levels(rng, extent, cuts, -0.22, 0.18) * result
    return jnp.clip(result, min=-reach, max=reach).astype(dtype)


def setup_inputs(seed: int = 0, part: int = 0) -> dict:
    arg_keys = jax.random.split(jax.random.key(seed), 8)
    part_keys = jax.random.split(jax.random.fold_in(arg_keys[7], part), 8)
    tokens = draw_tokens(jax.random.fold_in(jax.random.fold_in(arg_keys[7], part), 71), part)
    w_forget = bell_draw(arg_keys[1], (D, ATTENTION_UNITS * DK), D ** -0.5, 0.09375, ((0, 4), (1, 4)))
    w_value = bell_draw(arg_keys[2], (D, ATTENTION_UNITS * DV), D ** -0.5, 0.09375, ((0, 4), (1, 4)))
    lower_bound = draw_lower_bound(jax.random.fold_in(arg_keys[7], 71), part)
    decay_shift = draw_decay_shift(jax.random.fold_in(jax.random.fold_in(arg_keys[7], part), 71), part)
    queries = bell_draw(part_keys[5], (INPUT_SEQUENCES, ATTENTION_UNITS * DK), 1.0, 6.0, ((1, 4),))
    read_gain = jnp.clip(1.0 + 0.18 * jax.random.normal(arg_keys[6], (ATTENTION_UNITS * DV,), jnp.float32), 0.1, 1.9)
    return {"tokens": tokens, "w_forget": w_forget, "w_value": w_value, "lower_bound": lower_bound, "decay_shift": decay_shift, "queries": queries, "read_gain": read_gain}


def one_sequence(tok_rows, shift_rows, w_forget, w_value, lower_bound):
    pre_gate = jnp.dot(tok_rows, w_forget, preferred_element_type=jnp.float32)
    values = jnp.dot(tok_rows, w_value, preferred_element_type=jnp.float32).astype(jnp.bfloat16)
    low_bound = lower_bound[None, :]
    log_forget = jnp.logaddexp(jnp.log(low_bound), jnp.log1p(-low_bound) + jax.nn.log_sigmoid(pre_gate))
    log_forget = log_forget.reshape(SEQUENCE_SPAN, ATTENTION_UNITS, DK) + shift_rows[:, :, None]
    key_gates = ((1.0 - low_bound) * jax.nn.sigmoid(-pre_gate)).reshape(SEQUENCE_SPAN, ATTENTION_UNITS, DK)
    span_count = SEQUENCE_SPAN // SPAN
    blocked = log_forget.reshape(span_count, SPAN, ATTENTION_UNITS, DK)
    inclusive = jnp.cumsum(blocked, axis=1)
    totals = inclusive[:, -1]
    weighted = (key_gates.reshape(span_count, SPAN, ATTENTION_UNITS, DK) * jnp.exp(totals[:, None] - inclusive)).astype(jnp.bfloat16)
    span_values = values.reshape(span_count, SPAN, ATTENTION_UNITS, DV)
    span_states = jnp.einsum('bthk,bthv->bhkv', weighted.astype(jnp.float32), span_values.astype(jnp.float32))
    suffix = jnp.cumsum(totals[::-1], axis=0)[::-1] - totals
    return lax.optimization_barrier(jnp.sum(jnp.exp(suffix)[..., None] * span_states, axis=0))

def reference(tokens, w_forget, w_value, lower_bound, decay_shift, queries, read_gain):

    def per_prompt(operands):
        return one_sequence(operands[0], operands[1], w_forget, w_value, lower_bound)
    final_state = lax.map(per_prompt, (tokens, decay_shift))
    cache_out = final_state.reshape(INPUT_SEQUENCES, ATTENTION_UNITS, DK * DV).astype(jnp.bfloat16)
    query_act = jax.nn.silu(queries.astype(jnp.float32)).reshape(INPUT_SEQUENCES, ATTENTION_UNITS, DK)
    total_read = jnp.einsum('shk,shkv->shv', query_act, final_state, precision=lax.Precision.HIGHEST)
    scaled = total_read * lax.rsqrt(lax.optimization_barrier(jnp.mean(total_read * total_read, axis=-1, keepdims=True)) + 1e-06)
    first_read = (scaled * read_gain.reshape(ATTENTION_UNITS, DV)).reshape(INPUT_SEQUENCES, ATTENTION_UNITS * DV).astype(jnp.bfloat16)
    return (cache_out, first_read)
```

```python
import functools

import jax
import jax.numpy as jnp
from jax import lax
from jax.experimental import pallas as pl
from jax.experimental.pallas import tpu as pltpu
from jax.sharding import PartitionSpec as P

DK = 128
DV = 128


def entering(part, axis, combine, identity):
    count = lax.axis_size(axis)
    place = lax.axis_index(axis)
    ahead = count - 1 - place
    gathered = lax.all_gather(part, axis)
    state = jnp.zeros_like(part) + jnp.asarray(identity, part.dtype)

    def one(turn, state):
        source = count - 1 - turn
        return combine(state, lax.dynamic_index_in_dim(gathered, source, 0, False))

    return lax.fori_loop(0, ahead, one, state)


def add_terms(earlier, later_part):
    return earlier + later_part


def shards(tokens, w_forget, w_value, lower_bound, decay_shift, queries, read_gain):
    seq_count, span_len, feat_width = tokens.shape
    tok_rows = tokens.reshape(seq_count * span_len, feat_width)
    head_local = lower_bound.shape[0] // DK
    sp_count = lax.axis_size("sp")
    own_rows = DK // sp_count
    pre_gate = jnp.dot(
        tok_rows,
        lax.all_gather(w_forget, "sp", axis=0, tiled=True),
        preferred_element_type=jnp.float32,
    )
    value_sum = jnp.dot(
        tok_rows,
        lax.all_gather(w_value, "sp", axis=0, tiled=True),
        preferred_element_type=jnp.float32,
    )
    values = value_sum.astype(jnp.bfloat16)
    low_bound = lower_bound[None, :]
    log_forget = jnp.logaddexp(
        jnp.log(low_bound), jnp.log1p(-low_bound) + jax.nn.log_sigmoid(pre_gate)
    )
    log_forget = log_forget.reshape(seq_count, span_len, head_local, DK) + decay_shift[..., None]
    key_gates = ((1.0 - low_bound) * jax.nn.sigmoid(-pre_gate)).reshape(
        seq_count, span_len, head_local, DK
    )
    inclusive = jnp.cumsum(log_forget, axis=1)
    totals = inclusive[:, -1]
    weighted = (key_gates * jnp.exp(totals[:, None] - inclusive)).astype(jnp.bfloat16)
    span_values = values.reshape(seq_count, span_len, head_local, DV)
    local_state = jnp.einsum(
        "sthk,sthv->shkv", weighted, span_values, preferred_element_type=jnp.float32
    )
    suffix = entering(totals, "sp", add_terms, jnp.zeros_like(totals))
    decayed = (jnp.exp(suffix)[..., None] * local_state).reshape(seq_count, head_local, DK * DV)
    final_state = lax.psum_scatter(
        decayed.astype(jnp.bfloat16), "sp", scatter_dimension=2, tiled=True
    ).astype(jnp.float32)
    cache_out = final_state.astype(jnp.bfloat16)
    query_act = jax.nn.silu(queries.astype(jnp.float32)).reshape(seq_count, head_local, DK)
    own_query = lax.dynamic_slice_in_dim(query_act, lax.axis_index("sp") * own_rows, own_rows, 2)
    partial_value = jnp.sum(
        own_query[..., None] * final_state.reshape(seq_count, head_local, own_rows, DV), axis=2
    )
    total_read = lax.psum(partial_value, "sp")
    scaled = total_read * lax.rsqrt(
        jnp.mean(total_read * total_read, axis=-1, keepdims=True) + 1e-06
    )
    first_read = (
        (scaled * read_gain.reshape(head_local, DV))
        .reshape(seq_count, head_local * DV)
        .astype(jnp.bfloat16)
    )
    return (cache_out, first_read)


SUB = 4


def remote(src, dst, send_sem, recv_sem, **device):
    return pltpu.make_async_remote_copy(
        src_ref=src,
        dst_ref=dst,
        send_sem=send_sem,
        recv_sem=recv_sem,
        device_id=device,
        device_id_type=pl.DeviceIdType.MESH,
    )


def kernel(
    spans, tok_in, wf_in, wv_in, shift_in, low_ref, query_ref, gain_ref, cache_ref, read_ref,
    tok, w_buf, shift, states, totals, out_send, out_recv, read_send, read_recv,
    local_sem, z_send, z_recv, x_send, x_recv, d_send, d_recv,
    w_send, w_recv, y_send, y_recv, s_send, s_recv, o_send, o_recv, r_send, r_recv,
):
    grp, z, tp = lax.axis_index("grp"), lax.axis_index("sp"), lax.axis_index("tp")
    x_tp = tp + 2 - 4 * (tp // 2)
    c_tp = tp + 1 - 2 * lax.rem(tp, 2)
    xc_tp = x_tp + 1 - 2 * lax.rem(tp, 2)
    seqs, span_len, _ = tok_in.shape
    k_rows = wf_in.shape[0]
    width = w_buf.shape[1] // 2
    heads = width // DK
    own_rows = DK // spans
    sub_rows = span_len // SUB
    steps = (spans - 1) * SUB

    def rows_of(src):
        return pl.ds(pl.multiple_of(src * k_rows, k_rows), k_rows)

    def cols_of(j):
        return pl.ds(pl.multiple_of(j * width, width), width)

    locals_ = [
        pltpu.make_async_copy(tok_in, tok.at[z], local_sem.at[0]),
        pltpu.make_async_copy(wf_in.at[:, cols_of(z)], w_buf.at[rows_of(z), pl.ds(0, width)], local_sem.at[1]),
        pltpu.make_async_copy(wv_in.at[:, cols_of(z)], w_buf.at[rows_of(z), pl.ds(width, width)], local_sem.at[2]),
        pltpu.make_async_copy(shift_in, shift.at[z], local_sem.at[3]),
    ]
    for c in locals_:
        c.start()

    barrier = pltpu.get_barrier_semaphore()
    for off in range(1, spans):
        pl.semaphore_signal(barrier, inc=1, device_id={"sp": lax.rem(z + off, spans)}, device_id_type=pl.DeviceIdType.MESH)
    pl.semaphore_signal(barrier, inc=1, device_id={"tp": x_tp}, device_id_type=pl.DeviceIdType.MESH)
    pl.semaphore_signal(barrier, inc=1, device_id={"tp": c_tp}, device_id_type=pl.DeviceIdType.MESH)
    pl.semaphore_signal(barrier, inc=1, device_id={"grp": 1 - grp}, device_id_type=pl.DeviceIdType.MESH)
    pl.semaphore_wait(barrier, spans + 2)

    def shift_copy(off):
        return remote(shift_in, shift.at[z], s_send.at[off - 1], s_recv.at[z], sp=lax.rem(z + off, spans))

    def weight_copy(w_in, off):
        to = lax.rem(z + off, spans)
        return remote(
            w_in.at[:, cols_of(to)], w_buf.at[rows_of(z), cols_of(grp)], w_send.at[off - 1], w_recv.at[z], sp=to
        )

    def weight_pass(src):
        part = w_buf.at[rows_of(src), cols_of(grp)]
        return remote(part, part, y_send.at[src], y_recv.at[src], grp=1 - grp)

    def piece(src, who, u):
        return tok.at[src, who, pl.ds(pl.multiple_of(u * sub_rows, sub_rows), sub_rows)]

    def z_copy(direction, src, u, to, from_input=False):
        here = piece(src, tp, u)
        start = tok_in.at[tp, pl.ds(pl.multiple_of(u * sub_rows, sub_rows), sub_rows)] if from_input else here
        return remote(start, here, z_send.at[direction, src, u], z_recv.at[src, u], sp=to)

    def x_copy(src, u):
        here = piece(src, tp, u)
        return remote(here, here, x_send.at[src, u], x_recv.at[src, u], tp=x_tp)

    def d_copy(kind, src, u):
        here = piece(src, tp if kind == 0 else x_tp, u)
        return remote(here, here, d_send.at[kind, src, u], d_recv.at[kind, src, u], tp=c_tp)

    for off in range(1, spans):
        shift_copy(off).start()

    @pl.when(grp == 0)
    def _():
        for off in range(1, spans):
            weight_copy(wf_in, off).start()

    @pl.when(grp == 1)
    def _():
        for off in range(1, spans):
            weight_copy(wv_in, off).start()

    signs = (1, -1)

    def fits(place):
        return jnp.logical_and(place >= 0, place < spans)

    for direction, sign in enumerate(signs):
        @pl.when(fits(z + sign))
        def _():
            def one(u, carry):
                z_copy(direction, z, u, z + sign, True).start()
                return carry

            lax.fori_loop(0, SUB, one, 0)

    for off in range(1, spans):
        src = lax.rem(z + off, spans)
        remote(wf_in.at[:, cols_of(0)], w_buf.at[rows_of(src), cols_of(grp)], w_send.at[off - 1], w_recv.at[src], sp=src).wait_recv()
        weight_pass(src).start()
    for off in range(1, spans):
        src = lax.rem(z + off, spans)
        remote(shift_in, shift.at[src], s_send.at[off - 1], s_recv.at[src], sp=src).wait_recv()
    for c in locals_:
        c.wait()

    low = low_ref[:, cols_of(z)]
    head_count = shift_in.shape[1]
    pick = (
        lax.broadcasted_iota(jnp.int32, (head_count, width), 0)
        == z * heads + lax.broadcasted_iota(jnp.int32, (head_count, width), 1) // DK
    ).astype(jnp.float32)
    later_mask = (
        lax.broadcasted_iota(jnp.int32, (span_len, span_len), 1)
        > lax.broadcasted_iota(jnp.int32, (span_len, span_len), 0)
    ).astype(jnp.float32)
    exact = lax.Precision.HIGHEST

    def compute(src, s):
        both = jnp.dot(tok[src, s], w_buf[...], preferred_element_type=jnp.float32)
        gates = (1.0 - low) * jax.nn.sigmoid(-both[:, :width])
        decay = jnp.log1p(-gates) + lax.dot_general(
            shift[src, s], pick, (((0,), (0,)), ((), ())), precision=exact, preferred_element_type=jnp.float32
        )
        later = jnp.dot(later_mask, decay, precision=exact, preferred_element_type=jnp.float32)
        totals[src, s] = jnp.broadcast_to(jnp.sum(decay, axis=0, keepdims=True), (8, width))
        weighted = (gates * jnp.exp(later)).astype(jnp.bfloat16)
        vals = both[:, width:].astype(jnp.bfloat16)
        for h in range(heads):
            lanes = slice(h * DK, (h + 1) * DK)
            states[src, s, h] = lax.dot_general(
                vals[:, lanes], weighted[:, lanes], (((0,), (0,)), ((), ())), preferred_element_type=jnp.float32
            )

    def stage(n, carry):
        far, u = n // SUB + 1, lax.rem(n, SUB)
        for direction, sign in enumerate(signs):
            src = z - far * sign

            @pl.when(jnp.logical_and(n < steps, fits(src)))
            def _():
                z_copy(direction, src, u, z - sign).wait_recv()

                @pl.when(fits(z + sign))
                def _():
                    z_copy(direction, src, u, z + sign).start()

                x_copy(src, u).start()
                d_copy(0, src, u).start()

        last = jnp.maximum(n - 1, 0)
        last_far, last_u = last // SUB + 1, lax.rem(last, SUB)
        for direction, sign in enumerate(signs):
            last_src = z - last_far * sign

            @pl.when(jnp.logical_and(jnp.logical_and(n >= 1, n <= steps), fits(last_src)))
            def _():
                here = piece(last_src, x_tp, last_u)
                remote(here, here, x_send.at[last_src, last_u], x_recv.at[last_src, last_u], tp=x_tp).wait_recv()
                d_copy(1, last_src, last_u).start()

        @pl.when(n == 1)
        def _():
            for off in range(1, spans):
                src = lax.rem(z + off, spans)
                part = w_buf.at[rows_of(src), cols_of(1 - grp)]
                remote(part, part, y_send.at[src], y_recv.at[src], grp=1 - grp).wait_recv()

        back = n - 1
        done_far, slot = back // SUB, lax.rem(back, SUB)
        who = jnp.where(slot == 0, tp, jnp.where(slot == 1, x_tp, jnp.where(slot == 2, c_tp, xc_tp)))

        def one_side(direction, inner):
            done_src = z - done_far * (1 - 2 * direction)
            real = jnp.logical_and(fits(done_src), jnp.logical_or(done_far > 0, direction == 0))

            @pl.when(jnp.logical_and(real, n >= 1))
            def _():
                for kind in range(2):
                    @pl.when(jnp.logical_and(done_far > 0, slot == 2 + kind))
                    def _():
                        for v in range(SUB):
                            here = piece(done_src, c_tp if kind == 0 else xc_tp, v)
                            remote(here, here, d_send.at[kind, done_src, v], d_recv.at[kind, done_src, v], tp=c_tp).wait_recv()

                compute(done_src, who)

            return inner

        return lax.fori_loop(0, 2, one_side, carry)

    lax.fori_loop(0, spans * SUB + 1, stage, 0)

    for s in range(seqs):
        query = query_ref[pl.ds(s, 1), cols_of(z)]
        query = query * jax.nn.sigmoid(query)
        for h in range(heads):
            lanes = slice(h * DK, (h + 1) * DK)
            suffix = jnp.zeros((1, DK), jnp.float32)
            turned = states[spans - 1, s, h]
            for b in range(spans - 2, -1, -1):
                suffix = suffix + totals[b + 1, s, 0:1, lanes]
                turned = turned + jnp.exp(suffix) * states[b, s, h]
            final = turned.T
            for j in range(spans):
                out_send[j, s, h] = final[j * own_rows:(j + 1) * own_rows].astype(jnp.bfloat16)
            total = jnp.dot(query[:, lanes], final, precision=exact, preferred_element_type=jnp.float32)
            scaled = total * lax.rsqrt(jnp.mean(total * total, axis=-1, keepdims=True) + 1e-06)
            first = pl.multiple_of(z * width + h * DV, DV)
            read_send[pl.ds(s, 1), lanes] = scaled * gain_ref[:, pl.ds(first, DV)]

    def out_copy(off):
        to = lax.rem(z + off, spans)
        return remote(out_send.at[to], out_recv.at[z], o_send.at[off - 1], o_recv.at[z], sp=to)

    def read_copy(off):
        return remote(read_send, read_recv.at[z], r_send.at[off - 1], r_recv.at[z], sp=lax.rem(z + off, spans))

    for off in range(1, spans):
        out_copy(off).start()
        read_copy(off).start()

    for off in range(1, spans):
        shift_copy(off).wait_send()
        weight_copy(wf_in, off).wait_send()
        weight_pass(lax.rem(z + off, spans)).wait_send()

    def drain(n, carry):
        far, u = n // SUB, lax.rem(n, SUB)
        for direction, sign in enumerate(signs):
            src = z - far * sign

            @pl.when(jnp.logical_and(fits(src), fits(z + sign)))
            def _():
                z_copy(direction, src, u, z + sign).wait_send()

            @pl.when(jnp.logical_and(fits(src), far > 0))
            def _():
                x_copy(src, u).wait_send()
                d_copy(0, src, u).wait_send()
                d_copy(1, src, u).wait_send()

        return carry

    lax.fori_loop(0, spans * SUB, drain, 0)

    for off in range(1, spans):
        src = lax.rem(z + off, spans)
        remote(out_send.at[src], out_recv.at[src], o_send.at[off - 1], o_recv.at[src], sp=src).wait_recv()
        remote(read_send, read_recv.at[src], r_send.at[off - 1], r_recv.at[src], sp=src).wait_recv()
    for src in range(spans):
        mine = z == src
        cache_ref[:, src * heads:(src + 1) * heads] = jnp.where(mine, out_send[src], out_recv[src])
        read_ref[:, src * width:(src + 1) * width] = jnp.where(mine, read_send[:seqs], read_recv[src, :seqs]).astype(jnp.bfloat16)
    for off in range(1, spans):
        out_copy(off).wait_send()
        read_copy(off).wait_send()


def fused(spans, tokens, w_forget, w_value, lower_bound, decay_shift, queries, read_gain):
    seqs, span_len, feat = tokens.shape
    k_rows, cols = w_forget.shape
    width = cols // spans
    heads = width // DK
    own_rows = DK // spans
    head_local = cols // DK
    anywhere = pl.BlockSpec(memory_space=pl.ANY)
    vmem = pl.BlockSpec(memory_space=pltpu.VMEM)
    dma = pltpu.SemaphoreType.DMA
    cache, read = pl.pallas_call(
        functools.partial(kernel, spans),
        out_shape=(
            jax.ShapeDtypeStruct((seqs, head_local, own_rows, DV), jnp.bfloat16),
            jax.ShapeDtypeStruct((seqs, cols), jnp.bfloat16),
        ),
        in_specs=[anywhere] * 3 + [vmem] * 4,
        out_specs=(vmem, vmem),
        scratch_shapes=[
            pltpu.VMEM((spans, seqs, span_len, feat), jnp.bfloat16),
            pltpu.VMEM((feat, 2 * width), jnp.bfloat16),
            pltpu.VMEM((spans, seqs, head_local, span_len), jnp.float32),
            pltpu.VMEM((spans, seqs, heads, DV, DK), jnp.float32),
            pltpu.VMEM((spans, seqs, 8, width), jnp.float32),
            pltpu.VMEM((spans, seqs, heads, own_rows, DV), jnp.bfloat16),
            pltpu.VMEM((spans, seqs, heads, own_rows, DV), jnp.bfloat16),
            pltpu.VMEM((8, width), jnp.float32),
            pltpu.VMEM((spans, 8, width), jnp.float32),
            dma((4,)),
            dma((2, spans, SUB)),
            dma((spans, SUB)),
            dma((spans, SUB)),
            dma((spans, SUB)),
            dma((2, spans, SUB)),
            dma((2, spans, SUB)),
            dma((spans - 1,)),
            dma((spans,)),
            dma((spans,)),
            dma((spans,)),
            dma((spans - 1,)),
            dma((spans,)),
            dma((spans - 1,)),
            dma((spans,)),
            dma((spans - 1,)),
            dma((spans,)),
        ],
        compiler_params=pltpu.CompilerParams(
            collective_id=0, has_side_effects=True, vmem_limit_bytes=60 * 1024 * 1024
        ),
        name="gated_state",
    )(
        tokens,
        w_forget,
        w_value,
        decay_shift.transpose(0, 2, 1),
        lower_bound.reshape(1, -1),
        queries.astype(jnp.float32),
        read_gain.reshape(1, -1),
    )
    return cache.reshape(seqs, head_local, own_rows * DV), read


def by_shape(tokens, w_forget, *rest):
    spans, lanes, groups = (lax.axis_size(a) for a in ("sp", "tp", "grp"))
    seqs, span_len, _ = tokens.shape
    heads = w_forget.shape[1] // DK
    fit = groups == 2 and lanes == 4 and seqs == lanes and heads % spans == 0
    fit = fit and DK % (16 * spans) == 0 and heads % 8 == 0 and span_len == DK
    if fit:
        return fused(spans, tokens, w_forget, *rest)
    return shards(tokens, w_forget, *rest)


def solution(mesh):
    placed = (
        P("grp", "sp", None),
        P("sp", "tp"),
        P("sp", "tp"),
        P("tp"),
        P("grp", "sp", "tp"),
        P("grp", "tp"),
        P("tp"),
    )
    return jax.shard_map(
        by_shape,
        mesh=mesh,
        in_specs=placed,
        out_specs=(P("grp", "tp", "sp"), P("grp", "tp")),
        check_vma=False,
    )
```

```python
import functools

import jax
import jax.numpy as jnp
from jax import lax
from jax.experimental import pallas as pl
from jax.experimental.pallas import tpu as pltpu
from jax.sharding import PartitionSpec as P

DK = 128
DV = 128


def entering(part, axis, combine, identity):
    count = lax.axis_size(axis)
    place = lax.axis_index(axis)
    ahead = count - 1 - place
    gathered = lax.all_gather(part, axis)
    state = jnp.zeros_like(part) + jnp.asarray(identity, part.dtype)

    def one(turn, state):
        source = count - 1 - turn
        return combine(state, lax.dynamic_index_in_dim(gathered, source, 0, False))

    return lax.fori_loop(0, ahead, one, state)


def add_terms(earlier, later_part):
    return earlier + later_part


def shards(tokens, w_forget, w_value, lower_bound, decay_shift, queries, read_gain):
    seq_count, span_len, feat_width = tokens.shape
    tok_rows = tokens.reshape(seq_count * span_len, feat_width)
    head_local = lower_bound.shape[0] // DK
    sp_count = lax.axis_size("sp")
    own_rows = DK // sp_count
    pre_gate = jnp.dot(
        tok_rows,
        lax.all_gather(w_forget, "sp", axis=0, tiled=True),
        preferred_element_type=jnp.float32,
    )
    value_sum = jnp.dot(
        tok_rows,
        lax.all_gather(w_value, "sp", axis=0, tiled=True),
        preferred_element_type=jnp.float32,
    )
    values = value_sum.astype(jnp.bfloat16)
    low_bound = lower_bound[None, :]
    log_forget = jnp.logaddexp(
        jnp.log(low_bound), jnp.log1p(-low_bound) + jax.nn.log_sigmoid(pre_gate)
    )
    log_forget = log_forget.reshape(seq_count, span_len, head_local, DK) + decay_shift[..., None]
    key_gates = ((1.0 - low_bound) * jax.nn.sigmoid(-pre_gate)).reshape(
        seq_count, span_len, head_local, DK
    )
    inclusive = jnp.cumsum(log_forget, axis=1)
    totals = inclusive[:, -1]
    weighted = (key_gates * jnp.exp(totals[:, None] - inclusive)).astype(jnp.bfloat16)
    span_values = values.reshape(seq_count, span_len, head_local, DV)
    local_state = jnp.einsum(
        "sthk,sthv->shkv", weighted, span_values, preferred_element_type=jnp.float32
    )
    suffix = entering(totals, "sp", add_terms, jnp.zeros_like(totals))
    decayed = (jnp.exp(suffix)[..., None] * local_state).reshape(seq_count, head_local, DK * DV)
    final_state = lax.psum_scatter(
        decayed.astype(jnp.bfloat16), "sp", scatter_dimension=2, tiled=True
    ).astype(jnp.float32)
    cache_out = final_state.astype(jnp.bfloat16)
    query_act = jax.nn.silu(queries.astype(jnp.float32)).reshape(seq_count, head_local, DK)
    own_query = lax.dynamic_slice_in_dim(query_act, lax.axis_index("sp") * own_rows, own_rows, 2)
    partial_value = jnp.sum(
        own_query[..., None] * final_state.reshape(seq_count, head_local, own_rows, DV), axis=2
    )
    total_read = lax.psum(partial_value, "sp")
    scaled = total_read * lax.rsqrt(
        jnp.mean(total_read * total_read, axis=-1, keepdims=True) + 1e-06
    )
    first_read = (
        (scaled * read_gain.reshape(head_local, DV))
        .reshape(seq_count, head_local * DV)
        .astype(jnp.bfloat16)
    )
    return (cache_out, first_read)


SUB = 4


def remote(src, dst, send_sem, recv_sem, **device):
    return pltpu.make_async_remote_copy(
        src_ref=src,
        dst_ref=dst,
        send_sem=send_sem,
        recv_sem=recv_sem,
        device_id=device,
        device_id_type=pl.DeviceIdType.MESH,
    )


def kernel(
    spans, tok_in, wf_in, wv_in, shift_in, low_ref, query_ref, gain_ref, cache_ref, read_ref,
    tok, w_buf, shift, states, totals, out_send, out_recv, read_send, read_recv,
    local_sem, z_send, z_recv, x_send, x_recv, d_send, d_recv,
    w_send, w_recv, y_send, y_recv, s_send, s_recv, o_send, o_recv, r_send, r_recv,
):
    grp, z, tp = lax.axis_index("grp"), lax.axis_index("sp"), lax.axis_index("tp")
    x_tp = tp + 2 - 4 * (tp // 2)
    c_tp = tp + 1 - 2 * lax.rem(tp, 2)
    xc_tp = x_tp + 1 - 2 * lax.rem(tp, 2)
    seqs, span_len, _ = tok_in.shape
    k_rows = wf_in.shape[0]
    width = w_buf.shape[1] // 2
    heads = width // DK
    own_rows = DK // spans
    sub_rows = span_len // SUB
    steps = (spans - 1) * SUB

    def rows_of(src):
        return pl.ds(pl.multiple_of(src * k_rows, k_rows), k_rows)

    def cols_of(j):
        return pl.ds(pl.multiple_of(j * width, width), width)

    locals_ = [
        pltpu.make_async_copy(tok_in, tok.at[z], local_sem.at[0]),
        pltpu.make_async_copy(wf_in.at[:, cols_of(z)], w_buf.at[rows_of(z), pl.ds(0, width)], local_sem.at[1]),
        pltpu.make_async_copy(wv_in.at[:, cols_of(z)], w_buf.at[rows_of(z), pl.ds(width, width)], local_sem.at[2]),
        pltpu.make_async_copy(shift_in, shift.at[z], local_sem.at[3]),
    ]
    for c in locals_:
        c.start()

    barrier = pltpu.get_barrier_semaphore()
    for off in range(1, spans):
        pl.semaphore_signal(barrier, inc=1, device_id={"sp": lax.rem(z + off, spans)}, device_id_type=pl.DeviceIdType.MESH)
    pl.semaphore_signal(barrier, inc=1, device_id={"tp": x_tp}, device_id_type=pl.DeviceIdType.MESH)
    pl.semaphore_signal(barrier, inc=1, device_id={"tp": c_tp}, device_id_type=pl.DeviceIdType.MESH)
    pl.semaphore_signal(barrier, inc=1, device_id={"grp": 1 - grp}, device_id_type=pl.DeviceIdType.MESH)
    pl.semaphore_wait(barrier, spans + 2)

    def shift_copy(off):
        return remote(shift_in, shift.at[z], s_send.at[off - 1], s_recv.at[z], sp=lax.rem(z + off, spans))

    def weight_copy(w_in, off):
        to = lax.rem(z + off, spans)
        return remote(
            w_in.at[:, cols_of(to)], w_buf.at[rows_of(z), cols_of(grp)], w_send.at[off - 1], w_recv.at[z], sp=to
        )

    def weight_pass(src):
        part = w_buf.at[rows_of(src), cols_of(grp)]
        return remote(part, part, y_send.at[src], y_recv.at[src], grp=1 - grp)

    def piece(src, who, u):
        return tok.at[src, who, pl.ds(pl.multiple_of(u * sub_rows, sub_rows), sub_rows)]

    def z_copy(direction, src, u, to, from_input=False):
        here = piece(src, tp, u)
        start = tok_in.at[tp, pl.ds(pl.multiple_of(u * sub_rows, sub_rows), sub_rows)] if from_input else here
        return remote(start, here, z_send.at[direction, src, u], z_recv.at[src, u], sp=to)

    def x_copy(src, u):
        here = piece(src, tp, u)
        return remote(here, here, x_send.at[src, u], x_recv.at[src, u], tp=x_tp)

    def d_copy(kind, src, u):
        here = piece(src, tp if kind == 0 else x_tp, u)
        return remote(here, here, d_send.at[kind, src, u], d_recv.at[kind, src, u], tp=c_tp)

    for off in range(1, spans):
        shift_copy(off).start()

    @pl.when(grp == 0)
    def _():
        for off in range(1, spans):
            weight_copy(wf_in, off).start()

    @pl.when(grp == 1)
    def _():
        for off in range(1, spans):
            weight_copy(wv_in, off).start()

    signs = (1, -1)

    def fits(place):
        return jnp.logical_and(place >= 0, place < spans)

    for direction, sign in enumerate(signs):
        @pl.when(fits(z + sign))
        def _():
            def one(u, carry):
                z_copy(direction, z, u, z + sign, True).start()
                return carry

            lax.fori_loop(0, SUB, one, 0)

    def pass_weights(far):
        for sign in signs:
            src = z - far * sign

            @pl.when(fits(src))
            def _():
                part = w_buf.at[rows_of(src), cols_of(grp)]
                remote(wf_in.at[:, cols_of(0)], part, w_send.at[0], w_recv.at[src], sp=z - sign).wait_recv()
                weight_pass(src).start()

    at_end = jnp.logical_or(z == 0, z == spans - 1)

    def far_of(block, sign):
        near = z - sign
        late = jnp.logical_or(near == 0, near == spans - 1)
        return block + 1 - jnp.where(late, 1, 0)

    low = low_ref[:, cols_of(z)]
    head_count = shift_in.shape[1]
    pick = (
        lax.broadcasted_iota(jnp.int32, (head_count, width), 0)
        == z * heads + lax.broadcasted_iota(jnp.int32, (head_count, width), 1) // DK
    ).astype(jnp.float32)
    later_mask = (
        lax.rem(lax.broadcasted_iota(jnp.int32, (span_len, 3 * span_len), 1), span_len)
        > lax.broadcasted_iota(jnp.int32, (span_len, 3 * span_len), 0)
    ).astype(jnp.float32).astype(jnp.bfloat16)
    exact = lax.Precision.HIGHEST

    def compute(src, first):
        rows = tok[src, pl.ds(first, 2)].reshape(2 * span_len, tok.shape[-1])
        both = jnp.dot(rows, w_buf[...], preferred_element_type=jnp.float32)
        for i in range(2):
            s = first + i
            mine = both[i * span_len:(i + 1) * span_len]
            gates = (1.0 - low) * jax.nn.sigmoid(-mine[:, :width])
            decay = jnp.log1p(-gates) + lax.dot_general(
                shift[src, s], pick, (((0,), (0,)), ((), ())), precision=exact, preferred_element_type=jnp.float32
            )
            parts, left = [], decay
            for _ in range(3):
                parts.append(left.astype(jnp.bfloat16))
                left = left - parts[-1].astype(jnp.float32)
            later = jnp.dot(later_mask, jnp.concatenate(parts, axis=0), preferred_element_type=jnp.float32)
            totals[src, s] = jnp.broadcast_to(jnp.sum(decay, axis=0, keepdims=True), (8, width))
            weighted = (gates * jnp.exp(later)).astype(jnp.bfloat16)
            vals = mine[:, width:].astype(jnp.bfloat16)
            for h in range(heads):
                lanes = slice(h * DK, (h + 1) * DK)
                states[src, s, h] = lax.dot_general(
                    vals[:, lanes], weighted[:, lanes], (((0,), (0,)), ((), ())), preferred_element_type=jnp.float32
                )

    def stage(n, carry):
        for far in range(1, spans):
            due = 0 if far == 1 else jnp.where(at_end, 2 * far - 3, 0)

            @pl.when(n == due)
            def _():
                pass_weights(far)

        block, u = n // SUB, lax.rem(n, SUB)
        for direction, sign in enumerate(signs):
            far = far_of(block, sign)
            src = z - far * sign

            @pl.when(jnp.logical_and(jnp.logical_and(n < steps, far > 0), fits(src)))
            def _():
                z_copy(direction, src, u, z - sign).wait_recv()

                @pl.when(fits(z + sign))
                def _():
                    z_copy(direction, src, u, z + sign).start()

                x_copy(src, u).start()
                d_copy(0, src, u).start()

        last = jnp.maximum(n - 1, 0)
        last_u = lax.rem(last, SUB)
        for direction, sign in enumerate(signs):
            last_far = far_of(last // SUB, sign)
            last_src = z - last_far * sign

            @pl.when(jnp.logical_and(jnp.logical_and(n >= 1, n <= steps), jnp.logical_and(last_far > 0, fits(last_src))))
            def _():
                here = piece(last_src, x_tp, last_u)
                remote(here, here, x_send.at[last_src, last_u], x_recv.at[last_src, last_u], tp=x_tp).wait_recv()
                d_copy(1, last_src, last_u).start()

        @pl.when(n == SUB)
        def _():
            for off in range(1, spans):
                src = lax.rem(z + off, spans)
                part = w_buf.at[rows_of(src), cols_of(1 - grp)]
                remote(part, part, y_send.at[src], y_recv.at[src], grp=1 - grp).wait_recv()
                remote(shift_in, shift.at[src], s_send.at[off - 1], s_recv.at[src], sp=src).wait_recv()
            for c in locals_:
                c.wait()

        kind = u // 2
        pair = 2 * lax.rem(tp // 2 + kind, 2)

        def one_side(side, inner):
            done_far = jnp.where(side == 2, 0, far_of(block - 1, 1 - 2 * side))
            done_src = z - done_far * (1 - 2 * side)
            real = jnp.logical_or(
                jnp.logical_and(side == 2, block == 1),
                jnp.logical_and(jnp.logical_and(side < 2, done_far > 0), fits(done_src)),
            )

            @pl.when(jnp.logical_and(jnp.logical_and(real, n >= SUB), lax.rem(u, 2) == 1))
            def _():
                @pl.when(side < 2)
                def _():
                    for v in range(SUB):
                        here = piece(done_src, c_tp + (xc_tp - c_tp) * kind, v)
                        remote(here, here, d_send.at[kind, done_src, v], d_recv.at[kind, done_src, v], tp=c_tp).wait_recv()

                compute(done_src, pair)

            return inner

        return lax.fori_loop(0, 3, one_side, carry)

    lax.fori_loop(0, spans * SUB, stage, 0)

    query_all = query_ref[:, cols_of(z)].astype(jnp.float32)
    query_all = query_all * jax.nn.sigmoid(query_all)
    for s in range(seqs):
        query = query_all[s:s + 1]
        for h in range(heads):
            lanes = slice(h * DK, (h + 1) * DK)
            suffix = jnp.zeros((1, DK), jnp.float32)
            turned = states[spans - 1, s, h]
            for b in range(spans - 2, -1, -1):
                suffix = suffix + totals[b + 1, s, 0:1, lanes]
                turned = turned + jnp.exp(suffix) * states[b, s, h]
            final = turned.T
            for j in range(spans):
                out_send[j, s, h] = final[j * own_rows:(j + 1) * own_rows].astype(jnp.bfloat16)
            total = jnp.dot(query[:, lanes], final, precision=exact, preferred_element_type=jnp.float32)
            scaled = total * lax.rsqrt(jnp.mean(total * total, axis=-1, keepdims=True) + 1e-06)
            first = pl.multiple_of(z * width + h * DV, DV)
            read_send[pl.ds(s, 1), lanes] = scaled * gain_ref[:, pl.ds(first, DV)]

    def out_copy(off):
        to = lax.rem(z + off, spans)
        return remote(out_send.at[to], out_recv.at[z], o_send.at[off - 1], o_recv.at[z], sp=to)

    def read_copy(off):
        return remote(read_send, read_recv.at[z], r_send.at[off - 1], r_recv.at[z], sp=lax.rem(z + off, spans))

    for off in range(1, spans):
        out_copy(off).start()
        read_copy(off).start()

    for off in range(1, spans):
        shift_copy(off).wait_send()
        weight_copy(wf_in, off).wait_send()
        weight_pass(lax.rem(z + off, spans)).wait_send()

    def drain(n, carry):
        far, u = n // SUB, lax.rem(n, SUB)
        for direction, sign in enumerate(signs):
            src = z - far * sign

            @pl.when(jnp.logical_and(fits(src), fits(z + sign)))
            def _():
                z_copy(direction, src, u, z + sign).wait_send()

            @pl.when(jnp.logical_and(fits(src), far > 0))
            def _():
                x_copy(src, u).wait_send()
                d_copy(0, src, u).wait_send()
                d_copy(1, src, u).wait_send()

        return carry

    lax.fori_loop(0, spans * SUB, drain, 0)

    for off in range(1, spans):
        src = lax.rem(z + off, spans)
        remote(out_send.at[src], out_recv.at[src], o_send.at[off - 1], o_recv.at[src], sp=src).wait_recv()
        remote(read_send, read_recv.at[src], r_send.at[off - 1], r_recv.at[src], sp=src).wait_recv()
    for src in range(spans):
        mine = z == src
        cache_ref[:, src * heads:(src + 1) * heads] = jnp.where(mine, out_send[src], out_recv[src])
        read_ref[:, src * width:(src + 1) * width] = jnp.where(mine, read_send[:seqs], read_recv[src, :seqs]).astype(jnp.bfloat16)
    for off in range(1, spans):
        out_copy(off).wait_send()
        read_copy(off).wait_send()


def fused(spans, tokens, w_forget, w_value, lower_bound, decay_shift, queries, read_gain):
    seqs, span_len, feat = tokens.shape
    k_rows, cols = w_forget.shape
    width = cols // spans
    heads = width // DK
    own_rows = DK // spans
    head_local = cols // DK
    anywhere = pl.BlockSpec(memory_space=pl.ANY)
    vmem = pl.BlockSpec(memory_space=pltpu.VMEM)
    dma = pltpu.SemaphoreType.DMA
    cache, read = pl.pallas_call(
        functools.partial(kernel, spans),
        out_shape=(
            jax.ShapeDtypeStruct((seqs, head_local, own_rows, DV), jnp.bfloat16),
            jax.ShapeDtypeStruct((seqs, cols), jnp.bfloat16),
        ),
        in_specs=[anywhere] * 3 + [vmem] * 4,
        out_specs=(vmem, vmem),
        scratch_shapes=[
            pltpu.VMEM((spans, seqs, span_len, feat), jnp.bfloat16),
            pltpu.VMEM((feat, 2 * width), jnp.bfloat16),
            pltpu.VMEM((spans, seqs, head_local, span_len), jnp.float32),
            pltpu.VMEM((spans, seqs, heads, DV, DK), jnp.float32),
            pltpu.VMEM((spans, seqs, 8, width), jnp.float32),
            pltpu.VMEM((spans, seqs, heads, own_rows, DV), jnp.bfloat16),
            pltpu.VMEM((spans, seqs, heads, own_rows, DV), jnp.bfloat16),
            pltpu.VMEM((8, width), jnp.float32),
            pltpu.VMEM((spans, 8, width), jnp.float32),
            dma((4,)),
            dma((2, spans, SUB)),
            dma((spans, SUB)),
            dma((spans, SUB)),
            dma((spans, SUB)),
            dma((2, spans, SUB)),
            dma((2, spans, SUB)),
            dma((spans - 1,)),
            dma((spans,)),
            dma((spans,)),
            dma((spans,)),
            dma((spans - 1,)),
            dma((spans,)),
            dma((spans - 1,)),
            dma((spans,)),
            dma((spans - 1,)),
            dma((spans,)),
        ],
        compiler_params=pltpu.CompilerParams(
            collective_id=0, has_side_effects=True, vmem_limit_bytes=60 * 1024 * 1024
        ),
        name="gated_state",
    )(
        tokens,
        w_forget,
        w_value,
        decay_shift.transpose(0, 2, 1),
        lower_bound.reshape(1, -1),
        queries,
        read_gain.reshape(1, -1),
    )
    return cache.reshape(seqs, head_local, own_rows * DV), read


def by_shape(tokens, w_forget, *rest):
    spans, lanes, groups = (lax.axis_size(a) for a in ("sp", "tp", "grp"))
    seqs, span_len, _ = tokens.shape
    heads = w_forget.shape[1] // DK
    fit = groups == 2 and lanes == 4 and seqs == lanes and heads % spans == 0
    fit = fit and DK % (16 * spans) == 0 and heads % 8 == 0 and span_len == DK
    if fit:
        return fused(spans, tokens, w_forget, *rest)
    return shards(tokens, w_forget, *rest)


def solution(mesh):
    placed = (
        P("grp", "sp", None),
        P("sp", "tp"),
        P("sp", "tp"),
        P("tp"),
        P("grp", "sp", "tp"),
        P("grp", "tp"),
        P("tp"),
    )
    return jax.shard_map(
        by_shape,
        mesh=mesh,
        in_specs=placed,
        out_specs=(P("grp", "tp", "sp"), P("grp", "tp")),
        check_vma=False,
    )
```
